512 devices in a mesh: grp: 2 (over y), sp: 32 (over z), tp: 8 (over x, core).
Axes of the slice: x: 4, y: 2, z: 32, core: 2. Of those that a mesh axis runs over, the one named last changes fastest.
The devices are a block of a 4x8x32 slice.
Arguments:
- inputs: bfloat16 [16384, 2048], P(('grp', 'sp')), parts along dimension 0, may hold values from -6 to 6
- norm_gain: float32 [2048], replicated, may hold values from 0.1 to 1.9
- da_query_weight: bfloat16 [2048, 1024], P('sp', 'tp'), may hold values from -0.125 to 0.125
- da_key_weight: bfloat16 [2048, 1024], P('sp', 'tp'), may hold values from -0.125 to 0.125
- da_value_weight: bfloat16 [2048, 1024], P('sp', 'tp'), may hold values from -0.125 to 0.125
- sw_query_weight: bfloat16 [2048, 1024], P('sp', 'tp'), may hold values from -0.125 to 0.125
- sw_key_weight: bfloat16 [2048, 512], P('sp', 'tp'), may hold values from -0.125 to 0.125
- sw_value_weight: bfloat16 [2048, 512], P('sp', 'tp'), may hold values from -0.125 to 0.125
- da_query_gain: float32 [64], replicated, may hold values from 0.6 to 30
- da_key_gain: float32 [64], replicated, may hold values from 0.6 to 30
- sw_query_gain: float32 [64], replicated, may hold values from 0.6 to 30
- sw_key_gain: float32 [64], replicated, may hold values from 0.6 to 30
- mix_lambda: float32 [8], P('tp'), may hold values from 0.3 to 0.8
- head_gain: float32 [128], replicated, may hold values from 0.1 to 1.9
- sink_logit: float32 [16], P('tp'), may hold values from 0 to 8
- da_out_weight: bfloat16 [1024, 2048], P('tp'), may hold values from -0.1875 to 0.1875
- sw_out_weight: bfloat16 [1024, 2048], P('tp'), may hold values from -0.1875 to 0.1875
Outputs:
- mixed: bfloat16 [16384, 2048], P(('grp', 'sp')), parts along dimension 0
The draws below stay inside these ranges and needn't reach their ends.
There are 2 independent parts, one for each index of `grp`. The reference program is written for one: setup_inputs(seed, part) draws one part's arguments, and reference() takes and returns one part's arrays. A program takes and returns all parts, laid end to end along the dimension named above; an argument that names none is the same for every part. Nothing has to cross between parts.
All inputs are finite; a program needn't handle non-finite values.
Results may differ from the reference program's by a relative error of at most 0.014.
The reference program's roundings to bfloat16 on the way count: a program that leaves them out, or rounds other values in their place, can miss the bound.
Values may be sent and summed in bfloat16 or wider, within the bound.
No kernel may reach another device: no remote copies, remote signals or barrier semaphores. Data moves between devices by JAX's collectives and lax.ppermute only.
A program may use at most 64 MiB of HBM per device.

```python
import math
import jax
import jax.numpy as jnp
from jax import lax

D = 2048
DA_HEADS = 8
SW_HEADS = 16
KV_HEADS = 8
HD = 64
WINDOW = 128
SEQ = 8192
N_TP = 8


def gain_draw(key, own):
    values = jax.random.uniform(jax.random.fold_in(key, own), (HD,), jnp.float32, 0.6, 2.4)
    return values


def draw_da_query_gain(key, part):
    return gain_draw(key, 11)


def draw_da_key_gain(key, part):
    return gain_draw(key, 12)


def draw_sw_query_gain(key, part):
    return gain_draw(key, 13)


def draw_sw_key_gain(key, part):
    return gain_draw(key, 14)


def level_of(key, extent, cuts, smallest, top_value):
    def one(dim, shards_of):
        steps = jax.random.uniform(jax.random.fold_in(jax.random.fold_in(key, 6), dim), (shards_of,), jnp.float32, smallest / len(cuts), top_value / len(cuts))
        return jnp.repeat(jnp.exp(steps), extent[dim] // shards_of).reshape((-1,) + (1,) * (len(extent) - dim - 1))

    loudness = one(*cuts[0])
    for cut in cuts[1:]:
        loudness = loudness * one(*cut)
    return loudness


def bell_draw(key, shape, width, reach, shards=(), held_as=jnp.bfloat16):
    entries = width * jax.random.normal(key, shape, jnp.float32)
    if shards:
        entries = entries * level_of(key, shape, shards, -0.22, 0.18)
    return jnp.clip(entries, -reach, reach).astype(held_as)


def setup_inputs(seed: int = 0, part: int = 0) -> dict:
    keys = jax.random.split(jax.random.key(seed), 18)
    own_keys = jax.random.split(jax.random.fold_in(keys[17], part), 18)
    inputs = bell_draw(own_keys[0], (SEQ, D), 1.0, 6.0, ((0, 32),))
    norm_gain = jnp.clip(1.0 + 0.18 * jax.random.normal(keys[1], (D,), jnp.float32), 0.1, 1.9)
    da_query_weight = bell_draw(keys[2], (D, DA_HEADS * 2 * HD), D ** -0.5, 0.125, ((0, 32), (1, 8)))
    da_key_weight = bell_draw(keys[3], (D, DA_HEADS * 2 * HD), D ** -0.5, 0.125, ((0, 32), (1, 8)))
    da_value_weight = bell_draw(keys[4], (D, DA_HEADS * 2 * HD), D ** -0.5, 0.125, ((0, 32), (1, 8)))
    sw_query_weight = bell_draw(keys[5], (D, SW_HEADS * HD), D ** -0.5, 0.125, ((0, 32), (1, 8)))
    sw_key_weight = bell_draw(keys[6], (D, KV_HEADS * HD), D ** -0.5, 0.125, ((0, 32), (1, 8)))
    sw_value_weight = bell_draw(keys[7], (D, KV_HEADS * HD), D ** -0.5, 0.125, ((0, 32), (1, 8)))
    da_query_gain = draw_da_query_gain(jax.random.fold_in(keys[17], 71), part)
    da_key_gain = draw_da_key_gain(jax.random.fold_in(keys[17], 71), part)
    sw_query_gain = draw_sw_query_gain(jax.random.fold_in(keys[17], 71), part)
    sw_key_gain = draw_sw_key_gain(jax.random.fold_in(keys[17], 71), part)
    mix_lambda = jnp.clip(0.3 + 0.5 * jax.random.uniform(keys[12], (DA_HEADS,), jnp.float32) ** level_of(keys[12], (DA_HEADS,), ((0, 8),), -0.2, 0.2), 0.3, 0.8)
    head_gain = jnp.clip(1.0 + 0.18 * jax.random.normal(keys[13], (2 * HD,), jnp.float32), 0.1, 1.9)
    sink_logit = jnp.clip(8.0 * jax.random.uniform(keys[14], (SW_HEADS,), jnp.float32) ** level_of(keys[14], (SW_HEADS,), ((0, 8),), -0.2, 0.2), 0.0, 8.0)
    da_out_weight = bell_draw(keys[15], (DA_HEADS * 2 * HD, D), (DA_HEADS * 2 * HD) ** -0.5, 0.1875, ((0, 8),))
    sw_out_weight = bell_draw(keys[16], (SW_HEADS * HD, D), (SW_HEADS * HD) ** -0.5, 0.1875, ((0, 8),))
    return {"inputs": inputs, "norm_gain": norm_gain, "da_query_weight": da_query_weight, "da_key_weight": da_key_weight, "da_value_weight": da_value_weight, "sw_query_weight": sw_query_weight, "sw_key_weight": sw_key_weight, "sw_value_weight": sw_value_weight, "da_query_gain": da_query_gain, "da_key_gain": da_key_gain, "sw_query_gain": sw_query_gain, "sw_key_gain": sw_key_gain, "mix_lambda": mix_lambda, "head_gain": head_gain, "sink_logit": sink_logit, "da_out_weight": da_out_weight, "sw_out_weight": sw_out_weight}


def rms_norm(values, gain):
    return values * lax.rsqrt(lax.optimization_barrier(jnp.mean(values * values, axis=-1, keepdims=True)) + 1e-06) * gain

def reference(inputs, norm_gain, da_query_weight, da_key_weight, da_value_weight, sw_query_weight, sw_key_weight, sw_value_weight, da_query_gain, da_key_gain, sw_query_gain, sw_key_gain, mix_lambda, head_gain, sink_logit, da_out_weight, sw_out_weight):
    length = inputs.shape[0]
    normed = rms_norm(inputs.astype(jnp.float32), norm_gain).astype(jnp.bfloat16)

    def project(matrix):
        return jnp.dot(normed, matrix, preferred_element_type=jnp.float32)
    da_query = rms_norm(project(da_query_weight).reshape(length, DA_HEADS, 2, HD), da_query_gain).astype(jnp.bfloat16)
    da_key = rms_norm(project(da_key_weight).reshape(length, DA_HEADS, 2, HD), da_key_gain).astype(jnp.bfloat16)
    da_value = project(da_value_weight).astype(jnp.bfloat16).reshape(length, DA_HEADS, 2 * HD)
    sw_query = rms_norm(project(sw_query_weight).reshape(length, SW_HEADS, HD), sw_query_gain).astype(jnp.bfloat16)
    sw_key = rms_norm(project(sw_key_weight).reshape(length, KV_HEADS, HD), sw_key_gain).astype(jnp.bfloat16)
    sw_value = project(sw_value_weight).astype(jnp.bfloat16).reshape(length, KV_HEADS, HD)
    scale = HD ** (-0.5)
    block = math.gcd(length, 512)
    positions = jnp.arange(length, dtype=jnp.int32)
    keys_wide = da_key.astype(jnp.float32)
    values_wide = da_value.astype(jnp.float32)

    def da_block(first):
        rows = lax.dynamic_slice_in_dim(da_query, first, block, 0).astype(jnp.float32)
        scores = jnp.einsum('qhmd,khmd->hmqk', rows, keys_wide) * scale
        here = first + jnp.arange(block, dtype=jnp.int32)
        scores = jnp.where(positions[None, :] <= here[:, None], scores, -jnp.inf)
        top = lax.optimization_barrier(jnp.max(scores, axis=-1, keepdims=True))
        weights = jnp.exp(scores - top)
        total = lax.optimization_barrier(jnp.sum(weights, axis=-1))
        rounded = lax.optimization_barrier(weights.astype(jnp.bfloat16)).astype(jnp.float32)
        summed = jnp.einsum('hmqk,khe->hmqe', rounded, values_wide)
        maps = summed / total[..., None]
        blend = maps[:, 0] - mix_lambda[:, None, None] * maps[:, 1]
        return jnp.transpose(blend, (1, 0, 2))
    starts = jnp.arange(length // block, dtype=jnp.int32) * block
    blend_all = lax.map(da_block, starts).reshape(length, DA_HEADS, 2 * HD)
    da_rows = rms_norm(blend_all, head_gain).astype(jnp.bfloat16).reshape(length, DA_HEADS * 2 * HD)
    groups = SW_HEADS // KV_HEADS
    count = length // WINDOW

    def band(array):
        tiles = array.astype(jnp.float32).reshape(count, WINDOW, KV_HEADS, HD)
        earlier = jnp.concatenate([jnp.zeros_like(tiles[:1]), tiles[:-1]], axis=0)
        return jnp.concatenate([earlier, tiles], axis=1)
    key_band = band(sw_key)
    value_band = band(sw_value)
    query_tiles = sw_query.astype(jnp.float32).reshape(count, WINDOW, KV_HEADS, groups, HD)
    scores = jnp.einsum('nqhgd,nkhd->nhgqk', query_tiles, key_band) * scale
    lag = WINDOW + jnp.arange(WINDOW)[:, None] - jnp.arange(2 * WINDOW)[None, :]
    key_places = jnp.arange(count)[:, None] * WINDOW - WINDOW + jnp.arange(2 * WINDOW)[None, :]
    valid = ((lag >= 0) & (lag < WINDOW))[None] & (key_places >= 0)[:, None, :]
    scores = jnp.where(valid[:, None, None], scores, -jnp.inf)
    sink = sink_logit.reshape(KV_HEADS, groups)[None, :, :, None]
    top = jnp.maximum(lax.optimization_barrier(jnp.max(scores, axis=-1)), sink)
    weights = jnp.exp(scores - top[..., None])
    total = lax.optimization_barrier(jnp.sum(weights, axis=-1)) + jnp.exp(sink - top)
    rounded = lax.optimization_barrier(weights.astype(jnp.bfloat16)).astype(jnp.float32)
    summed = jnp.einsum('nhgqk,nkhd->nqhgd', rounded, value_band)
    sw_rows = (summed / jnp.transpose(total, (0, 3, 1, 2))[..., None]).astype(jnp.bfloat16).reshape(length, SW_HEADS * HD)
    da_cols = DA_HEADS * 2 * HD // N_TP
    sw_cols = SW_HEADS * HD // N_TP
    mixed = jnp.zeros((length, D), jnp.float32)
    for member in range(N_TP):
        partial_value = jnp.dot(da_rows[:, member * da_cols:(member + 1) * da_cols], da_out_weight[member * da_cols:(member + 1) * da_cols], preferred_element_type=jnp.float32)
        partial_value = partial_value + jnp.dot(sw_rows[:, member * sw_cols:(member + 1) * sw_cols], sw_out_weight[member * sw_cols:(member + 1) * sw_cols], preferred_element_type=jnp.float32)
        mixed = mixed + lax.optimization_barrier(partial_value.astype(jnp.bfloat16)).astype(jnp.float32)
    return mixed.astype(jnp.bfloat16)
```

```python
import functools

import jax
import jax.numpy as jnp
from jax import lax
from jax.experimental import pallas as pl
from jax.experimental.pallas import tpu as pltpu
from jax.sharding import PartitionSpec as P

HD = 64
WINDOW = 128
EPS = 1e-06
CUBE = 4
SPARE = 8
STAT_ROWS = 16
NEG = -1e30
MIB = 1024 * 1024


def dot(a, b):
    return lax.dot_general(a, b, (((1,), (0,)), ((), ())), preferred_element_type=jnp.float32)


def dot_t(a, b):
    return lax.dot_general(a, b, (((1,), (1,)), ((), ())), preferred_element_type=jnp.float32)


def half_norm(values, gain):
    low = lax.broadcasted_iota(jnp.int32, values.shape, 1) < HD
    squares = values * values
    first = jnp.sum(jnp.where(low, squares, 0.0), axis=-1, keepdims=True) / HD
    second = jnp.sum(jnp.where(low, 0.0, squares), axis=-1, keepdims=True) / HD
    scale = jnp.where(low, lax.rsqrt(first + EPS), lax.rsqrt(second + EPS))
    return values * scale * gain


def project(place_ref, blocks_ref, pieces, width, rows):
    member = lax.rem(place_ref[0], CUBE)
    total = jnp.zeros((rows, width), jnp.float32)
    for slot, piece in enumerate(pieces):
        source = lax.rem(member - slot + CUBE, CUBE)
        total += dot(blocks_ref[source, :rows, :], piece[...])
    return total


def da_project_kernel(rows, place_ref, blocks_ref, w0, w1, w2, w3, gain_q, gain_k, q_ref, kv_ref, spare_ref):
    everything = blocks_ref.shape[1]
    total = project(place_ref, blocks_ref, (w0, w1, w2, w3), 6 * HD, everything)
    key = half_norm(total[:, : 2 * HD], gain_k[...]).astype(jnp.bfloat16)
    value = total[:, 2 * HD : 4 * HD].astype(jnp.bfloat16)
    q_ref[...] = half_norm(total[:rows, 4 * HD :], gain_q[...]).astype(jnp.bfloat16)
    sent = rows - SPARE
    kv_ref[:, : 2 * HD] = key[:sent]
    kv_ref[:, 2 * HD :] = value[:sent]
    spare_ref[:, : 2 * HD] = key[rows:]
    spare_ref[:, 2 * HD :] = value[rows:]


def sw_project_kernel(rows, place_ref, blocks_ref, w0, w1, w2, w3, gain_q, gain_k, q_ref, kv_ref):
    total = project(place_ref, blocks_ref, (w0, w1, w2, w3), 4 * HD, rows)
    q_ref[...] = half_norm(total[:, : 2 * HD], gain_q[...]).astype(jnp.bfloat16)
    kv = total[:, 2 * HD :]
    low = lax.broadcasted_iota(jnp.int32, kv.shape, 1) < HD
    kv_ref[...] = jnp.where(low, half_norm(kv, gain_k[...]), kv).astype(jnp.bfloat16)


def da_attend_kernel(first_ref, q_ref, kv_ref, places_ref, out_ref):
    rows = q_ref.shape[1]
    first = first_ref[pl.program_id(0)]
    query = q_ref[0]
    key = kv_ref[:, : 2 * HD]
    value = kv_ref[:, 2 * HD :]
    lane = lax.broadcasted_iota(jnp.int32, (rows, 2 * HD), 1)
    own = first + lax.broadcasted_iota(jnp.int32, (rows, 1), 0)
    valid = places_ref[...] <= own
    stats = jnp.zeros((rows, 2 * HD), jnp.float32)
    for m in range(2):
        mine = (lane < HD) if m == 0 else (lane >= HD)
        scores = dot_t(jnp.where(mine, query, jnp.zeros_like(query)), key) * HD ** (-0.5)
        scores = jnp.where(valid, scores, NEG)
        top = jnp.max(scores, axis=-1, keepdims=True)
        weights = jnp.exp(scores - top)
        total = jnp.sum(weights, axis=-1, keepdims=True)
        summed = dot(weights.astype(jnp.bfloat16), value)
        out_ref[0, :rows, m * 2 * HD : (m + 1) * 2 * HD] = (summed / total).astype(jnp.bfloat16)
        rest = top + jnp.log(total)
        for part in range(3):
            head = rest.astype(jnp.bfloat16).astype(jnp.float32)
            stats = jnp.where(lane == 3 * m + part, head, stats)
            rest = rest - head
    out_ref[0, rows:, :] = jnp.transpose(stats)[:STAT_ROWS].astype(jnp.bfloat16)


def merge_kernel(lambda_ref, a0, a1, a2, a3, gain_ref, out_ref):
    rows = out_ref.shape[0]
    pieces = (a0, a1, a2, a3)
    shares = []
    for m in range(2):
        logs = []
        for piece in pieces:
            stat = piece[rows:, :].astype(jnp.float32)
            logs.append(stat[3 * m : 3 * m + 1] + stat[3 * m + 1 : 3 * m + 2] + stat[3 * m + 2 : 3 * m + 3])
        top = functools.reduce(jnp.maximum, logs)
        weights = [jnp.exp(log - top) for log in logs]
        total = functools.reduce(jnp.add, weights)
        shares.extend(weight / total for weight in weights)
    table = jnp.concatenate(shares + [jnp.zeros((2 * HD - len(shares), rows), jnp.float32)], axis=0)
    columns = jnp.transpose(table)
    maps = []
    for m in range(2):
        summed = jnp.zeros((rows, 2 * HD), jnp.float32)
        for i, piece in enumerate(pieces):
            at = len(pieces) * m + i
            summed += columns[:, at : at + 1] * piece[:rows, m * 2 * HD : (m + 1) * 2 * HD].astype(jnp.float32)
        maps.append(summed)
    blend = maps[0] - lambda_ref[0] * maps[1]
    scale = lax.rsqrt(jnp.mean(blend * blend, axis=-1, keepdims=True) + EPS)
    out_ref[...] = (blend * scale * gain_ref[...]).astype(jnp.bfloat16)


def sw_attend_kernel(place_ref, sink_ref, q_ref, before_ref, own_ref, out_ref):
    rows = q_ref.shape[0]
    kv = jnp.concatenate([before_ref[...], own_ref[...]], axis=0)
    query = q_ref[...].astype(jnp.float32)
    low = lax.broadcasted_iota(jnp.int32, query.shape, 1) < HD
    shape = (rows, rows + WINDOW)
    column = lax.broadcasted_iota(jnp.int32, shape, 1)
    lag = WINDOW + lax.broadcasted_iota(jnp.int32, shape, 0) - column
    earliest = jnp.where(place_ref[0] == 0, WINDOW, 0)
    valid = (lag >= 0) & (lag < WINDOW) & (column >= earliest)
    outs = []
    for j in range(2):
        mine = query if j == 0 else pltpu.roll(query, HD, 1)
        scores = dot_t(jnp.where(low, mine, 0.0).astype(jnp.bfloat16), kv) * HD ** (-0.5)
        scores = jnp.where(valid, scores, NEG)
        sink = sink_ref[j]
        top = jnp.maximum(jnp.max(scores, axis=-1, keepdims=True), sink)
        weights = jnp.exp(scores - top)
        total = jnp.sum(weights, axis=-1, keepdims=True) + jnp.exp(sink - top)
        outs.append(dot(weights.astype(jnp.bfloat16), kv) / total)
    out_ref[...] = jnp.where(low, pltpu.roll(outs[0], HD, 1), outs[1]).astype(jnp.bfloat16)


def mix_kernel(core_ref, same_ref, other_ref, w_ref, out_ref):
    total = jnp.zeros(out_ref.shape, jnp.float32)
    core = core_ref[0]
    for chip in range(same_ref.shape[0]):
        for rows_ref, index in ((same_ref, 2 * chip + core), (other_ref, 2 * chip + 1 - core)):
            total += dot(rows_ref[chip], w_ref[index]).astype(jnp.bfloat16).astype(jnp.float32)
    out_ref[...] = total.astype(jnp.bfloat16)


SMEM = pl.BlockSpec(memory_space=pltpu.SMEM)
VMEM = pl.BlockSpec(memory_space=pltpu.VMEM)


def call(kernel, out_shape, specs, args, name, flops):
    return pl.pallas_call(
        kernel,
        out_shape=out_shape,
        in_specs=specs,
        name=name,
        cost_estimate=pl.CostEstimate(flops=flops, bytes_accessed=4 * MIB, transcendentals=0),
        compiler_params=pltpu.CompilerParams(vmem_limit_bytes=48 * MIB),
    )(*args)


def shape_of(*dims):
    return jax.ShapeDtypeStruct(dims, jnp.bfloat16)


def twice(gain):
    return jnp.concatenate([gain, gain])[None]


def in_cube(value, count, steps):
    pairs = [(z, z // CUBE * CUBE + (z + steps) % CUBE) for z in range(count)]
    return lax.ppermute(value, "sp", pairs)


def on_device(
    inputs,
    norm_gain,
    da_query_weight,
    da_key_weight,
    da_value_weight,
    sw_query_weight,
    sw_key_weight,
    sw_value_weight,
    da_query_gain,
    da_key_gain,
    sw_query_gain,
    sw_key_gain,
    mix_lambda,
    head_gain,
    sink_logit,
    da_out_weight,
    sw_out_weight,
):
    rows, width = inputs.shape
    depth = da_query_weight.shape[0]
    count = lax.axis_size("sp")
    groups = lax.axis_size("tp")
    cubes = count // CUBE
    place = lax.axis_index("sp").astype(jnp.int32)
    member = lax.rem(place, CUBE)
    place_arg = place.reshape(1)
    strided = [list(range(r, count, CUBE)) for r in range(CUBE)]

    out_weights = lax.all_gather(
        jnp.concatenate([da_out_weight, sw_out_weight], axis=0), "tp", axis=0, tiled=False
    )

    da_cols = 6 * HD
    sw_cols = 4 * HD
    shard = jnp.concatenate(
        [
            da_key_weight,
            da_value_weight,
            da_query_weight,
            sw_query_weight,
            sw_key_weight,
            sw_value_weight,
            inputs[rows - SPARE :].reshape(depth, SPARE * width // depth),
        ],
        axis=1,
    )
    gathered = lax.all_gather(shard, "sp", axis=0, tiled=True, axis_index_groups=strided)
    da_piece = gathered[:, :da_cols]
    sw_piece = gathered[:, da_cols : da_cols + sw_cols]
    spare_rows = gathered[:, da_cols + sw_cols :].reshape(cubes * SPARE, width)
    da_pieces = [da_piece] + [in_cube(da_piece, count, k) for k in range(1, CUBE)]

    everything = jnp.concatenate([inputs, spare_rows], axis=0).astype(jnp.float32)
    mean = jnp.mean(everything * everything, axis=-1, keepdims=True)
    normed = (everything * lax.rsqrt(mean + EPS) * norm_gain).astype(jnp.bfloat16)
    total_rows = rows + cubes * SPARE
    blocks = (
        normed.reshape(total_rows, cubes, CUBE, depth)
        .transpose(2, 0, 1, 3)
        .reshape(CUBE, total_rows, cubes * depth)
    )

    query, kv_sent, kv_spare = call(
        functools.partial(da_project_kernel, rows),
        (
            shape_of(rows, 2 * HD),
            shape_of(rows - SPARE, 4 * HD),
            shape_of(cubes * SPARE, 4 * HD),
        ),
        [SMEM] + [VMEM] * 7,
        (place_arg, blocks, *da_pieces, twice(da_query_gain), twice(da_key_gain)),
        "da_project",
        2 * total_rows * width * da_cols,
    )
    queries = jnp.stack([query] + [in_cube(query, count, k) for k in range(1, CUBE)])
    kv_far = lax.all_gather(kv_sent, "sp", axis=0, tiled=True, axis_index_groups=strided)
    kv = jnp.concatenate([kv_far, kv_spare], axis=0)

    cube = jnp.arange(cubes, dtype=jnp.int32)[:, None] * (CUBE * rows)
    far_places = (cube + jnp.arange(rows - SPARE, dtype=jnp.int32)[None]).reshape(-1)
    spare_places = (cube + jnp.arange(rows - SPARE, rows, dtype=jnp.int32)[None]).reshape(-1)
    places = (jnp.concatenate([far_places, spare_places]) + member * rows)[None]
    sources = lax.rem(member - jnp.arange(CUBE, dtype=jnp.int32) + CUBE, CUBE)
    firsts = (place - member + sources) * rows

    keys = kv.shape[0]
    partials = pl.pallas_call(
        da_attend_kernel,
        grid=(CUBE,),
        out_shape=shape_of(CUBE, rows + STAT_ROWS, 4 * HD),
        in_specs=[
            SMEM,
            pl.BlockSpec((1, rows, 2 * HD), lambda i: (i, 0, 0)),
            pl.BlockSpec((keys, 4 * HD), lambda i: (0, 0)),
            pl.BlockSpec((1, keys), lambda i: (0, 0)),
        ],
        out_specs=pl.BlockSpec((1, rows + STAT_ROWS, 4 * HD), lambda i: (i, 0, 0)),
        name="da_attend",
        cost_estimate=pl.CostEstimate(
            flops=8 * CUBE * rows * keys * 2 * HD, bytes_accessed=4 * MIB, transcendentals=0
        ),
        compiler_params=pltpu.CompilerParams(vmem_limit_bytes=48 * MIB),
    )(firsts, queries, kv, places)
    pieces = [partials[0]] + [in_cube(partials[k], count, -k) for k in range(1, CUBE)]

    sw_pieces = [sw_piece] + [in_cube(sw_piece, count, k) for k in range(1, CUBE)]
    sw_query, sw_kv = call(
        functools.partial(sw_project_kernel, rows),
        (shape_of(rows, 2 * HD), shape_of(rows, 2 * HD)),
        [SMEM] + [VMEM] * 7,
        (place_arg, blocks, *sw_pieces, twice(sw_query_gain), twice(sw_key_gain)),
        "sw_project",
        2 * rows * width * sw_cols,
    )
    before = lax.ppermute(
        sw_kv[rows - WINDOW :], "sp", [(z, z + 1) for z in range(count - 1)]
    )
    sw_rows = call(
        sw_attend_kernel,
        shape_of(rows, 2 * HD),
        [SMEM, SMEM] + [VMEM] * 3,
        (place_arg, sink_logit, sw_query, before, sw_kv),
        "sw_attend",
        16 * rows * (rows + WINDOW) * HD,
    )

    da_rows = call(
        merge_kernel,
        shape_of(rows, 2 * HD),
        [SMEM] + [VMEM] * 5,
        (mix_lambda, *pieces, head_gain[None]),
        "merge",
        32 * rows * 2 * HD,
    )

    both = jnp.concatenate([da_rows, sw_rows], axis=1)
    parity = [list(range(c, groups, 2)) for c in range(2)]
    same = lax.all_gather(both, "tp", axis=0, tiled=False, axis_index_groups=parity)
    other = lax.ppermute(same, "tp", [(t, t ^ 1) for t in range(groups)])
    core = lax.rem(lax.axis_index("tp").astype(jnp.int32), 2).reshape(1)
    columns = out_weights.shape[2]
    tile = 512
    return pl.pallas_call(
        mix_kernel,
        grid=(columns // tile,),
        out_shape=shape_of(rows, columns),
        in_specs=[
            SMEM,
            pl.BlockSpec(same.shape, lambda i: (0, 0, 0)),
            pl.BlockSpec(other.shape, lambda i: (0, 0, 0)),
            pl.BlockSpec(out_weights.shape[:2] + (tile,), lambda i: (0, 0, i)),
        ],
        out_specs=pl.BlockSpec((rows, tile), lambda i: (0, i)),
        name="mix",
        cost_estimate=pl.CostEstimate(
            flops=4 * groups * rows * 2 * HD * 2 * columns, bytes_accessed=10 * MIB, transcendentals=0
        ),
        compiler_params=pltpu.CompilerParams(vmem_limit_bytes=48 * MIB),
    )(core, same, other, out_weights)


def solution(mesh):
    return jax.shard_map(
        on_device,
        mesh=mesh,
        in_specs=(
            P(("grp", "sp"), None),
            P(),
            P("sp", "tp"),
            P("sp", "tp"),
            P("sp", "tp"),
            P("sp", "tp"),
            P("sp", "tp"),
            P("sp", "tp"),
            P(),
            P(),
            P(),
            P(),
            P("tp"),
            P(),
            P("tp"),
            P("tp", None),
            P("tp", None),
        ),
        out_specs=P(("grp", "sp"), None),
        check_vma=False,
    )
```

```python
import functools

import jax
import jax.numpy as jnp
from jax import lax
from jax.experimental import pallas as pl
from jax.experimental.pallas import tpu as pltpu
from jax.sharding import PartitionSpec as P

HD = 64
WINDOW = 128
EPS = 1e-06
CUBE = 4
SPARE = 1
STAT_ROWS = 16
NEG = -1e30
MIB = 1024 * 1024


def dot(a, b):
    return lax.dot_general(a, b, (((1,), (0,)), ((), ())), preferred_element_type=jnp.float32)


def dot_t(a, b):
    return lax.dot_general(a, b, (((1,), (1,)), ((), ())), preferred_element_type=jnp.float32)


def half_norm(values, gain):
    low = lax.broadcasted_iota(jnp.int32, values.shape, 1) < HD
    squares = values * values
    first = jnp.sum(jnp.where(low, squares, 0.0), axis=-1, keepdims=True) / HD
    second = jnp.sum(jnp.where(low, 0.0, squares), axis=-1, keepdims=True) / HD
    scale = jnp.where(low, lax.rsqrt(first + EPS), lax.rsqrt(second + EPS))
    return values * scale * gain


def project(place_ref, blocks_ref, pieces, rows):
    member = lax.rem(place_ref[0], CUBE)
    total = jnp.zeros((rows, pieces[0].shape[1]), jnp.float32)
    for slot, piece in enumerate(pieces):
        source = lax.rem(member - slot + CUBE, CUBE)
        total += dot(blocks_ref[source, :rows, :], piece[...])
    return total


def kv_project_kernel(rows, place_ref, blocks_ref, w0, w1, w2, w3, gain_k, kv_ref, spare_ref):
    total = project(place_ref, blocks_ref, (w0, w1, w2, w3), blocks_ref.shape[1])
    key = half_norm(total[:, : 2 * HD], gain_k[...]).astype(jnp.bfloat16)
    value = total[:, 2 * HD :].astype(jnp.bfloat16)
    sent = rows - SPARE
    kv_ref[:, : 2 * HD] = key[:sent]
    kv_ref[:, 2 * HD :] = value[:sent]
    spare_ref[:, : 2 * HD] = key[rows:]
    spare_ref[:, 2 * HD :] = value[rows:]


def q_project_kernel(place_ref, blocks_ref, w0, w1, w2, w3, gain_q, q_ref):
    total = project(place_ref, blocks_ref, (w0, w1, w2, w3), q_ref.shape[0])
    q_ref[...] = half_norm(total, gain_q[...]).astype(jnp.bfloat16)


def sw_project_kernel(place_ref, blocks_ref, w0, w1, w2, w3, gain_q, gain_k, q_ref, kv_ref):
    total = project(place_ref, blocks_ref, (w0, w1, w2, w3), q_ref.shape[0])
    q_ref[...] = half_norm(total[:, : 2 * HD], gain_q[...]).astype(jnp.bfloat16)
    kv = total[:, 2 * HD :]
    low = lax.broadcasted_iota(jnp.int32, kv.shape, 1) < HD
    kv_ref[...] = jnp.where(low, half_norm(kv, gain_k[...]), kv).astype(jnp.bfloat16)


def da_attend_kernel(first_ref, q_ref, kv_ref, places_ref, out_ref):
    rows = q_ref.shape[0]
    first = first_ref[0]
    query = q_ref[...]
    key = kv_ref[:, : 2 * HD]
    value = kv_ref[:, 2 * HD :]
    lane = lax.broadcasted_iota(jnp.int32, (rows, 2 * HD), 1)
    own = first + lax.broadcasted_iota(jnp.int32, (rows, 1), 0)
    valid = places_ref[...] <= own
    stats = jnp.zeros((rows, 2 * HD), jnp.float32)
    for m in range(2):
        mine = (lane < HD) if m == 0 else (lane >= HD)
        scores = dot_t(jnp.where(mine, query, jnp.zeros_like(query)), key) * HD ** (-0.5)
        scores = jnp.where(valid, scores, NEG)
        top = jnp.max(scores, axis=-1, keepdims=True)
        weights = jnp.exp(scores - top)
        total = jnp.sum(weights, axis=-1, keepdims=True)
        summed = dot(weights.astype(jnp.bfloat16), value)
        out_ref[:rows, m * 2 * HD : (m + 1) * 2 * HD] = (summed / total).astype(jnp.bfloat16)
        rest = top + jnp.log(total)
        for part in range(3):
            head = rest.astype(jnp.bfloat16).astype(jnp.float32)
            stats = jnp.where(lane == 3 * m + part, head, stats)
            rest = rest - head
    out_ref[rows:, :] = jnp.transpose(stats)[:STAT_ROWS].astype(jnp.bfloat16)


def merge_kernel(lambda_ref, a0, a1, a2, a3, gain_ref, out_ref):
    rows = out_ref.shape[0]
    pieces = (a0, a1, a2, a3)
    shares = []
    for m in range(2):
        logs = []
        for piece in pieces:
            stat = piece[rows:, :].astype(jnp.float32)
            logs.append(stat[3 * m : 3 * m + 1] + stat[3 * m + 1 : 3 * m + 2] + stat[3 * m + 2 : 3 * m + 3])
        top = functools.reduce(jnp.maximum, logs)
        weights = [jnp.exp(log - top) for log in logs]
        total = functools.reduce(jnp.add, weights)
        shares.extend(weight / total for weight in weights)
    table = jnp.concatenate(shares + [jnp.zeros((2 * HD - len(shares), rows), jnp.float32)], axis=0)
    columns = jnp.transpose(table)
    maps = []
    for m in range(2):
        summed = jnp.zeros((rows, 2 * HD), jnp.float32)
        for i, piece in enumerate(pieces):
            at = len(pieces) * m + i
            summed += columns[:, at : at + 1] * piece[:rows, m * 2 * HD : (m + 1) * 2 * HD].astype(jnp.float32)
        maps.append(summed)
    blend = maps[0] - lambda_ref[0] * maps[1]
    scale = lax.rsqrt(jnp.mean(blend * blend, axis=-1, keepdims=True) + EPS)
    out_ref[...] = (blend * scale * gain_ref[...]).astype(jnp.bfloat16)


def sw_attend_kernel(place_ref, sink_ref, q_ref, before_ref, own_ref, out_ref):
    rows = q_ref.shape[0]
    kv = jnp.concatenate([before_ref[...], own_ref[...]], axis=0)
    query = q_ref[...].astype(jnp.float32)
    low = lax.broadcasted_iota(jnp.int32, query.shape, 1) < HD
    shape = (rows, rows + WINDOW)
    column = lax.broadcasted_iota(jnp.int32, shape, 1)
    lag = WINDOW + lax.broadcasted_iota(jnp.int32, shape, 0) - column
    earliest = jnp.where(place_ref[0] == 0, WINDOW, 0)
    valid = (lag >= 0) & (lag < WINDOW) & (column >= earliest)
    outs = []
    for j in range(2):
        mine = query if j == 0 else pltpu.roll(query, HD, 1)
        scores = dot_t(jnp.where(low, mine, 0.0).astype(jnp.bfloat16), kv) * HD ** (-0.5)
        scores = jnp.where(valid, scores, NEG)
        sink = sink_ref[j]
        top = jnp.maximum(jnp.max(scores, axis=-1, keepdims=True), sink)
        weights = jnp.exp(scores - top)
        total = jnp.sum(weights, axis=-1, keepdims=True) + jnp.exp(sink - top)
        outs.append(dot(weights.astype(jnp.bfloat16), kv) / total)
    out_ref[...] = jnp.where(low, pltpu.roll(outs[0], HD, 1), outs[1]).astype(jnp.bfloat16)


def mix_kernel(chip_ref, rows_ref, w0, w1, w2, w3, out_ref):
    chips = rows_ref.shape[0]
    total = jnp.zeros(out_ref.shape, jnp.float32)
    for slot, w_ref in enumerate((w0, w1, w2, w3)):
        source = lax.rem(chip_ref[0] - slot + chips, chips)
        total += dot(rows_ref[source], w_ref[...]).astype(jnp.bfloat16).astype(jnp.float32)
    out_ref[...] = total


SMEM = pl.BlockSpec(memory_space=pltpu.SMEM)
VMEM = pl.BlockSpec(memory_space=pltpu.VMEM)


def call(kernel, out_shape, specs, args, name, flops):
    return pl.pallas_call(
        kernel,
        out_shape=out_shape,
        in_specs=specs,
        name=name,
        cost_estimate=pl.CostEstimate(flops=flops, bytes_accessed=4 * MIB, transcendentals=0),
        compiler_params=pltpu.CompilerParams(vmem_limit_bytes=48 * MIB),
    )(*args)


def shape_of(*dims):
    return jax.ShapeDtypeStruct(dims, jnp.bfloat16)


def twice(gain):
    return jnp.concatenate([gain, gain])[None]


def in_cube(value, count, steps):
    pairs = [(z, z // CUBE * CUBE + (z + steps) % CUBE) for z in range(count)]
    return lax.ppermute(value, "sp", pairs)


def on_device(
    inputs,
    norm_gain,
    da_query_weight,
    da_key_weight,
    da_value_weight,
    sw_query_weight,
    sw_key_weight,
    sw_value_weight,
    da_query_gain,
    da_key_gain,
    sw_query_gain,
    sw_key_gain,
    mix_lambda,
    head_gain,
    sink_logit,
    da_out_weight,
    sw_out_weight,
):
    rows, width = inputs.shape
    depth = da_query_weight.shape[0]
    count = lax.axis_size("sp")
    groups = lax.axis_size("tp")
    cubes = count // CUBE
    place = lax.axis_index("sp").astype(jnp.int32)
    member = lax.rem(place, CUBE)
    place_arg = place.reshape(1)
    strided = [list(range(r, count, CUBE)) for r in range(CUBE)]

    kv_cols = 4 * HD
    q_cols = 2 * HD
    sw_cols = 4 * HD
    shard = jnp.concatenate(
        [
            da_key_weight,
            da_value_weight,
            da_query_weight,
            sw_query_weight,
            sw_key_weight,
            sw_value_weight,
            inputs[rows - SPARE :].reshape(depth, SPARE * width // depth),
        ],
        axis=1,
    )
    gathered = lax.all_gather(shard, "sp", axis=0, tiled=True, axis_index_groups=strided)
    at = [0, kv_cols, kv_cols + q_cols, kv_cols + q_cols + sw_cols]
    kv_piece, q_piece, sw_piece = (gathered[:, i:j] for i, j in zip(at, at[1:]))
    spare_rows = gathered[:, at[3] :].reshape(cubes * SPARE, width)
    kv_pieces = [kv_piece] + [in_cube(kv_piece, count, k) for k in range(1, CUBE)]

    everything = jnp.concatenate([inputs, spare_rows], axis=0).astype(jnp.float32)
    mean = jnp.mean(everything * everything, axis=-1, keepdims=True)
    q_piece, mean = lax.optimization_barrier((q_piece, mean))
    q_pieces = [q_piece] + [in_cube(q_piece, count, k) for k in range(1, CUBE)]
    normed = (everything * lax.rsqrt(mean + EPS) * norm_gain).astype(jnp.bfloat16)
    total_rows = rows + cubes * SPARE
    blocks = (
        normed.reshape(total_rows, cubes, CUBE, depth)
        .transpose(2, 0, 1, 3)
        .reshape(CUBE, total_rows, cubes * depth)
    )
    blocks, da_out_weight, sw_out_weight = lax.optimization_barrier(
        (blocks, da_out_weight, sw_out_weight)
    )
    out_weight = jnp.concatenate([da_out_weight, sw_out_weight], axis=0)
    out_weights = [out_weight] + [
        lax.ppermute(out_weight, "tp", [(t, (t + 2 * k) % groups) for t in range(groups)])
        for k in range(1, groups // 2)
    ]

    kv_sent, kv_spare = call(
        functools.partial(kv_project_kernel, rows),
        (shape_of(rows - SPARE, kv_cols), shape_of(cubes * SPARE, kv_cols)),
        [SMEM] + [VMEM] * 6,
        (place_arg, blocks, *kv_pieces, twice(da_key_gain)),
        "kv_project",
        2 * total_rows * width * kv_cols,
    )
    kv_far = lax.all_gather(kv_sent, "sp", axis=0, tiled=False, axis_index_groups=strided)
    kv_far, q_pieces = lax.optimization_barrier((kv_far, q_pieces))
    kv = jnp.concatenate([kv_far, kv_spare.reshape(cubes, SPARE, kv_cols)], axis=1)
    kv = kv.reshape(cubes * rows, kv_cols)

    query = call(
        q_project_kernel,
        shape_of(rows, q_cols),
        [SMEM] + [VMEM] * 6,
        (place_arg, blocks, *q_pieces, twice(da_query_gain)),
        "q_project",
        2 * rows * width * q_cols,
    )
    query, sw_piece = lax.optimization_barrier((query, sw_piece))
    queries = [query] + [in_cube(query, count, k) for k in range(1, CUBE)]
    sw_pieces = [sw_piece] + [in_cube(sw_piece, count, k) for k in range(1, CUBE)]
    sw_query, sw_kv = call(
        sw_project_kernel,
        (shape_of(rows, 2 * HD),) * 2,
        [SMEM] + [VMEM] * 7,
        (place_arg, blocks, *sw_pieces, twice(sw_query_gain), twice(sw_key_gain)),
        "sw_project",
        2 * rows * width * sw_cols,
    )

    cube = jnp.arange(cubes, dtype=jnp.int32)[:, None] * (CUBE * rows)
    places = (cube + jnp.arange(rows, dtype=jnp.int32)[None]).reshape(1, -1) + member * rows

    keys = kv.shape[0]
    partials = []
    for slot in range(CUBE):
        source = lax.rem(member - slot + CUBE, CUBE)
        partial = call(
            da_attend_kernel,
            shape_of(rows + STAT_ROWS, 4 * HD),
            [SMEM] + [VMEM] * 3,
            (((place - member + source) * rows).reshape(1), queries[slot], kv, places),
            "da_attend",
            8 * rows * keys * 2 * HD,
        )
        partials.append(in_cube(partial, count, -slot) if slot else partial)

    before = lax.ppermute(
        sw_kv[rows - WINDOW :], "sp", [(z, z + 1) for z in range(count - 1)]
    )
    sw_rows = call(
        sw_attend_kernel,
        shape_of(rows, 2 * HD),
        [SMEM, SMEM] + [VMEM] * 3,
        (place_arg, sink_logit, sw_query, before, sw_kv),
        "sw_attend",
        16 * rows * (rows + WINDOW) * HD,
    )

    da_rows = call(
        merge_kernel,
        shape_of(rows, 2 * HD),
        [SMEM] + [VMEM] * 5,
        (mix_lambda, *partials, head_gain[None]),
        "merge",
        32 * rows * 2 * HD,
    )

    both = jnp.concatenate([da_rows, sw_rows], axis=1)
    parity = [list(range(c, groups, 2)) for c in range(2)]
    near = lax.all_gather(both, "tp", axis=0, tiled=False, axis_index_groups=parity)
    chip = (lax.axis_index("tp").astype(jnp.int32) // 2).reshape(1)
    columns = out_weight.shape[1]
    tile = 512
    w_spec = pl.BlockSpec((out_weight.shape[0], tile), lambda i: (0, i))
    mine = pl.pallas_call(
        mix_kernel,
        grid=(columns // tile,),
        out_shape=jax.ShapeDtypeStruct((rows, columns), jnp.float32),
        in_specs=[SMEM, pl.BlockSpec(near.shape, lambda i: (0, 0, 0))] + [w_spec] * len(out_weights),
        out_specs=pl.BlockSpec((rows, tile), lambda i: (0, i)),
        name="mix",
        cost_estimate=pl.CostEstimate(
            flops=2 * groups * rows * 2 * HD * 2 * columns, bytes_accessed=8 * MIB, transcendentals=0
        ),
        compiler_params=pltpu.CompilerParams(vmem_limit_bytes=48 * MIB),
    )(chip, near, *out_weights)
    other = lax.ppermute(mine, "tp", [(t, t ^ 1) for t in range(groups)])
    return (mine + other).astype(jnp.bfloat16)


def solution(mesh):
    return jax.shard_map(
        on_device,
        mesh=mesh,
        in_specs=(
            P(("grp", "sp"), None),
            P(),
            P("sp", "tp"),
            P("sp", "tp"),
            P("sp", "tp"),
            P("sp", "tp"),
            P("sp", "tp"),
            P("sp", "tp"),
            P(),
            P(),
            P(),
            P(),
            P("tp"),
            P(),
            P("tp"),
            P("tp", None),
            P("tp", None),
        ),
        out_specs=P(("grp", "sp"), None),
        check_vma=False,
    )
```
